128 devices in a mesh: fs: 32 (over z, y, core), tp: 4 (over x).
Axes of the slice: x: 4, y: 4, z: 4, core: 2. Of those that a mesh axis runs over, the one named last changes fastest.
Arguments:
- x_saved: bfloat16 [65536, 2048], P('fs'), may hold values from -6 to 6
- h_saved: bfloat16 [65536, 1024], P('fs', 'tp'), may hold values from -6 to 6
- key_cot: bfloat16 [65536, 1024], P('fs', 'tp'), may hold values from -6 to 6
- value_cot: bfloat16 [65536, 1024], P('fs', 'tp'), may hold values from -6 to 6
- out_cot: bfloat16 [65536, 2048], P('fs'), may hold values from -6 to 6
- w_key: float32 [2048, 1024], P('fs', 'tp'), may hold values from -0.125 to 0.125
- w_value: float32 [2048, 1024], P('fs', 'tp'), may hold values from -0.125 to 0.125
- w_out: float32 [1024, 2048], P('tp', 'fs'), may hold values from -0.1875 to 0.1875
- p_key: bfloat16 [2048, 256], P('fs'), may hold values from -1 to 1, as said below
- p_value: bfloat16 [2048, 256], P('fs'), may hold values from -1 to 1, as said below
- p_out: bfloat16 [2048, 256], P('fs'), may hold values from -1 to 1, as said below
- m_key: float32 [2, 256, 1024], P(None, 'fs', 'tp'), may hold values from -1.5 to 1.5, as said below
- m_value: float32 [2, 256, 1024], P(None, 'fs', 'tp'), may hold values from -1.5 to 1.5, as said below
- m_out: float32 [2, 256, 1024], P(None, 'fs', 'tp'), may hold values from -1.5 to 1.5, as said below
Outputs:
- step_key: float32 [2048, 1024], P('fs', 'tp')
- step_value: float32 [2048, 1024], P('fs', 'tp')
- step_out: float32 [1024, 2048], P('tp', 'fs')
- copy_key: bfloat16 [2048, 1024], P(None, 'tp')
- copy_value: bfloat16 [2048, 1024], P(None, 'tp')
- copy_out: bfloat16 [1024, 2048], P('tp')
- new_m_key: float32 [2, 256, 1024], P(None, 'fs', 'tp')
- new_m_value: float32 [2, 256, 1024], P(None, 'fs', 'tp')
- new_m_out: float32 [2, 256, 1024], P(None, 'fs', 'tp')
The draws below stay inside these ranges and needn't reach their ends.
Inputs may be any that keep to these rules, and one draw needn't show every extreme that they name: `p_key`: factor entries are real-valued, dense and of full rank. `p_value`: factor entries are real-valued, dense and of full rank. `p_out`: factor entries are real-valued, dense and of full rank. `m_key`: plane 1 (second moments) lies in 0.05 to 1. `m_value`: plane 1 (second moments) lies in 0.05 to 1. `m_out`: plane 1 (second moments) lies in 0.05 to 1.
All inputs are finite; a program needn't handle non-finite values.
Results may differ from the reference program's by a relative error of at most 0.0085.
Values may be sent and summed in bfloat16 or wider, within the bound.
No kernel may reach another device: no remote copies, remote signals or barrier semaphores. Data moves between devices by JAX's collectives and lax.ppermute only.
A program may use at most 128 MiB of HBM per device.

```python
import math
import jax
import jax.numpy as jnp
from jax import lax

D = 2048
HW = 1024
RANK = 256
TOKENS = 65536


def factor_draw(key, member):
    key = jax.random.fold_in(key, member)
    key_base, key_cols = jax.random.split(key, 2)
    gaussian = jax.random.truncated_normal(key_base, -4.0, 4.0, (D, RANK), jnp.float32)
    columns = jnp.arange(RANK, dtype=jnp.float32)
    rising = 10.0 ** (columns / RANK) * jax.random.uniform(key_cols, (RANK,), jnp.float32, 0.7, 1.4)
    factor_values = gaussian * rising[None, :] * D ** (-0.5)
    return jnp.clip(factor_values, -1.0, 1.0).astype(jnp.bfloat16)


def moment_draw(key, member):
    key = jax.random.fold_in(key, member)
    key_one, key_two = jax.random.split(key)
    plane_one = 0.3 * jax.random.truncated_normal(key_one, -5.0, 5.0, (RANK, HW), jnp.float32)
    plane_two = jnp.exp(jax.random.uniform(key_two, (RANK, HW), jnp.float32, math.log(0.05), 0.0))
    return jnp.stack([plane_one, plane_two]).astype(jnp.float32)


def draw_p_key(key, part):
    return factor_draw(key, 11)


def draw_p_value(key, part):
    return factor_draw(key, 12)


def draw_p_out(key, part):
    return factor_draw(key, 13)


def draw_m_key(key, part):
    return moment_draw(key, 21)


def draw_m_value(key, part):
    return moment_draw(key, 22)


def draw_m_out(key, part):
    return moment_draw(key, 23)


def block_levels(rng, dims, pieces, smallest, top_value):
    def one(position, parts):
        draws = jax.random.uniform(jax.random.fold_in(jax.random.fold_in(rng, 6), position), (parts,), jnp.float32, smallest / len(pieces), top_value / len(pieces))
        return jnp.repeat(jnp.exp(draws), dims[position] // parts).reshape((-1,) + (1,) * (len(dims) - position - 1))

    loudness = one(*pieces[0])
    for cut in pieces[1:]:
        loudness = loudness * one(*cut)
    return loudness


def normal_values(key, extent, width, limit, cuts=(), kind=jnp.bfloat16):
    values = jax.random.normal(key, extent, jnp.float32) * width
    if len(cuts) > 0:
        values = block_levels(key, extent, cuts, -0.22, 0.18) * values
    return jnp.clip(values, min=-limit, max=limit).astype(kind)


def setup_inputs(seed: int = 0) -> dict:
    keys = jax.random.split(jax.random.key(seed), 15)
    x_saved = normal_values(keys[0], (TOKENS, D), 1.0, 6.0, ((0, 32),))
    h_saved = normal_values(keys[1], (TOKENS, HW), 1.0, 6.0, ((0, 32), (1, 4)))
    key_cot = normal_values(keys[2], (TOKENS, HW), 1.0, 6.0, ((0, 32), (1, 4)))
    value_cot = normal_values(keys[3], (TOKENS, HW), 1.0, 6.0, ((0, 32), (1, 4)))
    out_cot = normal_values(keys[4], (TOKENS, D), 1.0, 6.0, ((0, 32),))
    w_key = normal_values(keys[5], (D, HW), D ** -0.5, 0.125, ((0, 32), (1, 4)), jnp.float32)
    w_value = normal_values(keys[6], (D, HW), D ** -0.5, 0.125, ((0, 32), (1, 4)), jnp.float32)
    w_out = normal_values(keys[7], (HW, D), HW ** -0.5, 0.1875, ((0, 4), (1, 32)), jnp.float32)
    p_key = draw_p_key(jax.random.fold_in(keys[14], 71), 0)
    p_value = draw_p_value(jax.random.fold_in(keys[14], 71), 0)
    p_out = draw_p_out(jax.random.fold_in(keys[14], 71), 0)
    m_key = draw_m_key(jax.random.fold_in(keys[14], 71), 0)
    m_value = draw_m_value(jax.random.fold_in(keys[14], 71), 0)
    m_out = draw_m_out(jax.random.fold_in(keys[14], 71), 0)
    return dict(x_saved=x_saved, h_saved=h_saved, key_cot=key_cot, value_cot=value_cot, out_cot=out_cot, w_key=w_key, w_value=w_value, w_out=w_out, p_key=p_key, p_value=p_value, p_out=p_out, m_key=m_key, m_value=m_value, m_out=m_out)


beta_one = 0.9
beta_two = 0.9
learn_rate = 0.01

def exact_dot(left, right):
    return jnp.dot(left.astype(jnp.float32), right.astype(jnp.float32), precision=lax.Precision.HIGHEST)

def reference(x_saved, h_saved, key_cot, value_cot, out_cot, w_key, w_value, w_out, p_key, p_value, p_out, m_key, m_value, m_out):
    x_wide = x_saved.astype(jnp.float32).T
    grad_key = exact_dot(x_wide, key_cot)
    grad_value = exact_dot(x_wide, value_cot)
    grad_out_t = exact_dot(out_cot.astype(jnp.float32).T, h_saved)
    factors = (p_key, p_value, p_out)
    projected = [exact_dot(factors[0].astype(jnp.float32).T, grad_key), exact_dot(factors[1].astype(jnp.float32).T, grad_value), exact_dot(factors[2].astype(jnp.float32).T, grad_out_t)]
    total = jnp.sum(projected[0] * projected[0]) + jnp.sum(projected[1] * projected[1]) + jnp.sum(projected[2] * projected[2])
    norm_scale = jnp.sqrt(total / (3 * RANK * HW) + 1e-06)
    olds = (m_key, m_value, m_out)
    steps = []
    moments = []
    for member in range(3):
        normed = projected[member] / norm_scale
        moment_one = beta_one * olds[member][0] + (1 - beta_one) * normed
        moment_two = beta_two * olds[member][1] + (1 - beta_two) * normed * normed
        direction = (moment_one / jnp.sqrt(moment_two)).astype(jnp.bfloat16)
        steps.append(exact_dot(factors[member], direction))
        moments.append(jnp.stack([moment_one, moment_two]))
    step_key = steps[0]
    step_value = steps[1]
    step_out = steps[2].T
    copy_key = (w_key - learn_rate * step_key).astype(jnp.bfloat16)
    copy_value = (w_value - learn_rate * step_value).astype(jnp.bfloat16)
    copy_out = (w_out - learn_rate * step_out).astype(jnp.bfloat16)
    return (step_key, step_value, step_out, copy_key, copy_value, copy_out, moments[0], moments[1], moments[2])
```

```python
import jax
import jax.numpy as jnp
from jax import lax
from jax.experimental import pallas as pl
from jax.experimental.pallas import tpu as pltpu
from jax.sharding import Mesh
from jax.sharding import PartitionSpec as P

FS = ("fs_0", "fs_1", "fs_2")
FAR = ("fs_0", "fs_1")
CORE = "fs_2"
MIB = 1024 * 1024

beta_one = 0.9
beta_two = 0.9
learn_rate = 0.01


def vmem():
    return pl.BlockSpec(memory_space=pltpu.VMEM)


def smem():
    return pl.BlockSpec(memory_space=pltpu.SMEM)


def swap(value):
    return lax.ppermute(value, CORE, [(0, 1), (1, 0)])


def far_gather(value):
    copies = jnp.broadcast_to(value, (16, *value.shape))
    return lax.all_to_all(copies, FAR, 0, 0, tiled=True)


def split_kernel(core_ref, gk_ref, gv_ref, go_ref, keep_ref, send_ref):
    first = core_ref[0] == 0
    for member, g_ref in enumerate((gk_ref, gv_ref, go_ref)):
        rows = pl.ds(member * 256, 256)
        for pair in range(8):
            left = g_ref[:, pl.ds(pair * 256, 128)]
            right = g_ref[:, pl.ds(pair * 256 + 128, 128)]
            low_half = lax.broadcasted_iota(jnp.int32, left.shape, 1) < 64
            zero = jnp.where(low_half, left, pltpu.roll(right, 64, 1))
            one = jnp.where(low_half, pltpu.roll(left, 64, 1), right)
            columns = pl.ds(pair * 128, 128)
            keep_ref[rows, columns] = jnp.where(first, zero, one)
            send_ref[rows, columns] = jnp.where(first, one, zero)


def split_by_core(core, grads):
    half = jax.ShapeDtypeStruct((768, 1024), jnp.float32)
    return pl.pallas_call(
        split_kernel,
        out_shape=(half, half),
        in_specs=[smem(), vmem(), vmem(), vmem()],
        out_specs=(vmem(), vmem()),
        compiler_params=pltpu.CompilerParams(vmem_limit_bytes=40 * MIB),
        name="split_by_core",
    )(core, *grads)


def project_kernel(core_ref, keep_ref, recv_ref, p_ref, mine_ref, other_ref):
    core = core_ref[0]
    for member in range(3):
        cols = pl.ds(member * 256, 256)
        grad = keep_ref[cols, :] + recv_ref[cols, :]
        high = grad.astype(jnp.bfloat16)
        low = (grad - high.astype(jnp.float32)).astype(jnp.bfloat16)
        factor = p_ref[:, cols]
        turned = jnp.dot(high, factor, preferred_element_type=jnp.float32) + jnp.dot(
            low, factor, preferred_element_type=jnp.float32
        )
        rows = turned.T.reshape(16, 2, 8, 256)
        mine_ref[:, :, cols] = jnp.where(core == 0, rows[:, 0], rows[:, 1])
        other_ref[:, :, cols] = jnp.where(core == 0, rows[:, 1], rows[:, 0])


def project(core, keep, recv, factors):
    half = jax.ShapeDtypeStruct((16, 8, 768), jnp.float32)
    return pl.pallas_call(
        project_kernel,
        out_shape=(half, half),
        in_specs=[smem(), vmem(), vmem(), vmem()],
        out_specs=(vmem(), vmem()),
        compiler_params=pltpu.CompilerParams(vmem_limit_bytes=40 * MIB),
        name="project",
    )(core, keep, recv, factors)


def direction_of(proj, m_one, m_two, scale):
    normed = proj / scale
    first = beta_one * m_one + (1 - beta_one) * normed
    second = beta_two * m_two + (1 - beta_two) * normed * normed
    return first, second, (first / jnp.sqrt(second)).astype(jnp.bfloat16)


def finish_kernel(
    core_ref,
    scale_ref,
    proj_a_ref,
    proj_b_ref,
    m_a_ref,
    m_b_ref,
    p_a_ref,
    p_b_ref,
    w_a_ref,
    w_b_ref,
    p_own_ref,
    own_ref,
    m_own_ref,
    step_k_ref,
    step_v_ref,
    step_o_ref,
    copy_k_ref,
    copy_v_ref,
    copy_o_ref,
    new_m_ref,
    dir_ref,
):
    core = core_ref[0]
    scale = scale_ref[0]
    for proj_ref, m_ref, slot in ((proj_a_ref, m_a_ref, core), (proj_b_ref, m_b_ref, 1 - core)):
        direction = direction_of(
            proj_ref[...].astype(jnp.float32),
            m_ref[:, 0].astype(jnp.float32),
            m_ref[:, 1].astype(jnp.float32),
            scale,
        )[2]
        dir_ref[:, slot] = direction
    first, second, _ = direction_of(own_ref[...], m_own_ref[0], m_own_ref[1], scale)
    new_m_ref[0] = first
    new_m_ref[1] = second
    steps = (step_k_ref, step_v_ref, step_o_ref)
    for member, copy_ref in enumerate((copy_k_ref, copy_v_ref, copy_o_ref)):
        cols = pl.ds(member * 256, 256)
        direction = dir_ref[:, :, :, cols].reshape(256, 256)
        own_step = jnp.dot(p_own_ref[:, cols], direction, preferred_element_type=jnp.float32)
        steps[member][...] = own_step.T if member == 2 else own_step
        for p_ref, w_ref, slot in ((p_a_ref, w_a_ref, core), (p_b_ref, w_b_ref, 1 - core)):
            for part in range(4):
                chunk = pl.ds(part * 4, 4)
                factor = p_ref[chunk, :, cols].reshape(256, 256)
                step = jnp.dot(factor, direction, preferred_element_type=jnp.float32)
                weight = w_ref[chunk, :, cols].reshape(256, 256).astype(jnp.float32)
                fresh = (weight - learn_rate * step).astype(jnp.bfloat16)
                copy_ref[chunk, slot] = fresh.reshape(4, 64, 256)


def finish(core, scale, proj_a, proj_b, m_a, m_b, p_a, p_b, w_a, w_b, p_own, own, m_own):
    copies = jax.ShapeDtypeStruct((16, 2, 64, 256), jnp.bfloat16)
    out_shape = (
        jax.ShapeDtypeStruct((64, 256), jnp.float32),
        jax.ShapeDtypeStruct((64, 256), jnp.float32),
        jax.ShapeDtypeStruct((256, 64), jnp.float32),
        copies,
        copies,
        copies,
        jax.ShapeDtypeStruct((2, 8, 768), jnp.float32),
    )
    return pl.pallas_call(
        finish_kernel,
        out_shape=out_shape,
        in_specs=[smem(), smem()] + [vmem()] * 11,
        out_specs=tuple(vmem() for _ in out_shape),
        scratch_shapes=[pltpu.VMEM((16, 2, 8, 768), jnp.bfloat16)],
        compiler_params=pltpu.CompilerParams(vmem_limit_bytes=50 * MIB),
        name="finish",
    )(core, scale, proj_a, proj_b, m_a, m_b, p_a, p_b, w_a, w_b, p_own, own, m_own)


def turned_grad(right, left):
    return lax.dot_general(
        right, left, (((0,), (0,)), ((), ())), preferred_element_type=jnp.float32
    )


def body(
    x_saved,
    h_saved,
    key_cot,
    value_cot,
    out_cot,
    w_key,
    w_value,
    w_out,
    p_key,
    p_value,
    p_out,
    m_key,
    m_value,
    m_out,
):
    core = lax.axis_index(CORE).astype(jnp.int32).reshape(1)
    p_own = jnp.concatenate([p_key, p_value, p_out], axis=1)
    p_a = far_gather(p_own)
    grads = (
        turned_grad(key_cot, x_saved),
        turned_grad(value_cot, x_saved),
        turned_grad(h_saved, out_cot),
    )
    keep, send = split_by_core(core, grads)
    recv = swap(send)

    w_own = jnp.concatenate([w_key, w_value, w_out.T], axis=1).astype(jnp.bfloat16)
    m_own = jnp.concatenate([m_key, m_value, m_out], axis=2)
    m_small = m_own.astype(jnp.bfloat16).reshape(16, 768)
    wm_own = jnp.concatenate([w_own, m_small], axis=0)
    p_a, wm_own = lax.optimization_barrier((p_a, wm_own))
    wm_a = far_gather(wm_own)
    w_a = wm_a[:, :64]
    m_a = wm_a[:, 64:].reshape(16, 2, 8, 768)

    mine, other = project(core, keep, recv, p_a.reshape(1024, 768))
    paired = (mine + swap(other)).astype(jnp.bfloat16)
    pieces = lax.all_to_all(paired, FAR, 0, 0, tiled=True)
    own = jnp.sum(pieces.astype(jnp.float32), axis=0)
    p_b = swap(p_a)
    w_b = swap(w_a)
    m_b = swap(m_a)

    square = jnp.sum(own * own).reshape(1, 1, 1)
    squares = lax.all_to_all(
        jnp.broadcast_to(square, (64, 1, 1)), ("fs_0", "fs_1", "tp"), 0, 0, tiled=True
    )
    half_total = jnp.sum(squares).reshape(1, 1)
    total = (half_total + swap(half_total)).reshape(1)
    scale = jnp.sqrt(total / 786432 + 1e-06)
    proj_a = far_gather(own.astype(jnp.bfloat16))
    proj_b = swap(proj_a)
    step_key, step_value, step_out, copy_key, copy_value, copy_out, new_m = finish(
        core, scale, proj_a, proj_b, m_a, m_b, p_a, p_b, w_a, w_b, p_own, own, m_own
    )
    return (
        step_key,
        step_value,
        step_out,
        copy_key.reshape(2048, 256),
        copy_value.reshape(2048, 256),
        copy_out.reshape(2048, 256).T,
        new_m[:, :, :256],
        new_m[:, :, 256:512],
        new_m[:, :, 512:],
    )


def solution(mesh):
    split = Mesh(mesh.devices.reshape(4, 4, 2, mesh.shape["tp"]), ("fs_0", "fs_1", "fs_2", "tp"))
    in_specs = (
        P(FS, None),
        P(FS, "tp"),
        P(FS, "tp"),
        P(FS, "tp"),
        P(FS, None),
        P(FS, "tp"),
        P(FS, "tp"),
        P("tp", FS),
        P(FS, None),
        P(FS, None),
        P(FS, None),
        P(None, FS, "tp"),
        P(None, FS, "tp"),
        P(None, FS, "tp"),
    )
    out_specs = (
        P(FS, "tp"),
        P(FS, "tp"),
        P("tp", FS),
        P(None, "tp"),
        P(None, "tp"),
        P("tp", None),
        P(None, FS, "tp"),
        P(None, FS, "tp"),
        P(None, FS, "tp"),
    )
    return jax.shard_map(body, mesh=split, in_specs=in_specs, out_specs=out_specs, check_vma=False)
```

```python
import jax
import jax.numpy as jnp
from jax import lax
from jax.experimental import pallas as pl
from jax.experimental.pallas import tpu as pltpu
from jax.sharding import Mesh
from jax.sharding import PartitionSpec as P

FS = ("fs_0", "fs_1", "fs_2")
FAR = ("fs_0", "fs_1")
CORE = "fs_2"
MIB = 1024 * 1024

beta_one = 0.9
beta_two = 0.9
learn_rate = 0.01


def vmem():
    return pl.BlockSpec(memory_space=pltpu.VMEM)


def smem():
    return pl.BlockSpec(memory_space=pltpu.SMEM)


def shift(value, axis, by):
    size = lax.axis_size(axis)
    return lax.ppermute(value, axis, [(i, (i + by) % size) for i in range(size)])


def mirrored(value, axis, by):
    size = lax.axis_size(axis)
    pairs = []
    for place in range(size):
        pairs.append((place * 2, (place + by) % size * 2))
        pairs.append((place * 2 + 1, (place - by) % size * 2 + 1))
    return lax.ppermute(value, (axis, CORE), pairs)


def swap(value):
    return shift(value, CORE, 1)


def spread_kernel(a_ref, b_ref, c_ref, out_ref):
    for copy in range(16):
        for member, ref in enumerate((a_ref, b_ref, c_ref)):
            out_ref[copy, :, pl.ds(member * 256, 256)] = ref[...]


def spread(a, b, c):
    return pl.pallas_call(
        spread_kernel,
        out_shape=jax.ShapeDtypeStruct((16, 64, 768), jnp.bfloat16),
        in_specs=[vmem()] * 3,
        out_specs=vmem(),
        name="spread",
    )(a, b, c)


def split_lanes(grad, first, keep_ref, send_ref, rows, start):
    for pair in range(grad.shape[1] // 256):
        left = grad[:, pair * 256 : pair * 256 + 128]
        right = grad[:, pair * 256 + 128 : pair * 256 + 256]
        low_half = lax.broadcasted_iota(jnp.int32, left.shape, 1) < 64
        turned = pltpu.roll(jnp.where(low_half, right, left), 64, 1)
        zero = jnp.where(low_half, left, turned)
        one = jnp.where(low_half, turned, right)
        columns = pl.ds(start + pair * 128, 128)
        keep_ref[rows, columns] = jnp.where(first, zero, one)
        send_ref[rows, columns] = jnp.where(first, one, zero).astype(jnp.bfloat16)


TILE = 1024
TILES = 2048 // TILE


def grad_kernel(
    core_ref,
    k_ref,
    v_ref,
    h_ref,
    x_ref,
    o_ref,
    keep_ref,
    send_ref,
    narrow_ref,
    wide_ref,
    keep_buf,
    send_buf,
    narrow_sem,
    wide_sem,
    out_sem,
):
    narrow = [
        pltpu.make_async_copy(ref, narrow_ref.at[n], narrow_sem.at[n])
        for n, ref in enumerate((k_ref, v_ref, h_ref))
    ]
    wide = [
        pltpu.make_async_copy(
            ref.at[:, pl.ds(tile * TILE, TILE)],
            wide_ref.at[group, :, pl.ds(tile * TILE, TILE)],
            wide_sem.at[group * TILES + tile],
        )
        for group, ref in enumerate((x_ref, o_ref))
        for tile in range(TILES)
    ]
    narrow[0].start()
    wide[0].start()
    narrow[1].start()
    for copy in wide[1:TILES]:
        copy.start()
    narrow[2].start()
    for copy in wide[TILES:]:
        copy.start()
    first = core_ref[0] == 0
    outs = []
    for group, members in enumerate(((0, 1), (2,))):
        for tile in range(TILES):
            if tile == 0:
                narrow[members[0]].wait()
            wide[group * TILES + tile].wait()
            for member in members:
                if tile == 0 and member == 1:
                    narrow[1].wait()
                rows = pl.ds(member * 256, 256)
                grad = lax.dot_general(
                    narrow_ref[member],
                    wide_ref[group, :, pl.ds(tile * TILE, TILE)],
                    (((0,), (0,)), ((), ())),
                    preferred_element_type=jnp.float32,
                )
                split_lanes(grad, first, keep_buf, send_buf, rows, tile * TILE // 2)
        rows = pl.ds(members[0] * 256, len(members) * 256)
        for side, (buf, ref) in enumerate(((keep_buf, keep_ref), (send_buf, send_ref))):
            copy = pltpu.make_async_copy(
                buf.at[rows, :], ref.at[rows, :], out_sem.at[group * 2 + side]
            )
            copy.start()
            outs.append(copy)
    for copy in outs:
        copy.wait()


def hbm_only(value):
    return pltpu.with_memory_space_constraint(value, pltpu.HBM)


def in_hbm():
    return pl.BlockSpec(memory_space=pltpu.HBM)


def grad_halves(core, key_cot, value_cot, h_saved, x_saved, out_cot):
    return pl.pallas_call(
        grad_kernel,
        out_shape=(
            pltpu.HBM((768, 1024), jnp.float32),
            pltpu.HBM((768, 1024), jnp.bfloat16),
        ),
        in_specs=[smem()] + [in_hbm()] * 5,
        out_specs=(in_hbm(), in_hbm()),
        scratch_shapes=[
            pltpu.VMEM((3, 2048, 256), jnp.bfloat16),
            pltpu.VMEM((2, 2048, 2048), jnp.bfloat16),
            pltpu.VMEM((768, 1024), jnp.float32),
            pltpu.VMEM((768, 1024), jnp.bfloat16),
            pltpu.SemaphoreType.DMA((3,)),
            pltpu.SemaphoreType.DMA((2 * TILES,)),
            pltpu.SemaphoreType.DMA((4,)),
        ],
        compiler_params=pltpu.CompilerParams(vmem_limit_bytes=48 * MIB),
        name="grads",
    )(core, *[hbm_only(a) for a in (key_cot, value_cot, h_saved, x_saved, out_cot)])


def pair_kernel(keep_ref, recv_ref, parts_ref, keep_buf, sem):
    copies = []
    for member in range(3):
        rows = pl.ds(member * 256, 256)
        copies.append(
            pltpu.make_async_copy(keep_ref.at[rows, :], keep_buf.at[rows, :], sem.at[member])
        )
        copies[member].start()
    for member in range(3):
        rows = pl.ds(member * 256, 256)
        copies[member].wait()
        grad = keep_buf[rows, :] + recv_ref[rows, :].astype(jnp.float32)
        parts_ref[member] = grad.astype(jnp.bfloat16)


def pair_sum(keep, recv):
    return pl.pallas_call(
        pair_kernel,
        out_shape=jax.ShapeDtypeStruct((3, 256, 1024), jnp.bfloat16),
        in_specs=[in_hbm(), vmem()],
        out_specs=vmem(),
        scratch_shapes=[
            pltpu.VMEM((768, 1024), jnp.float32),
            pltpu.SemaphoreType.DMA((3,)),
        ],
        compiler_params=pltpu.CompilerParams(vmem_limit_bytes=12 * MIB),
        name="pair_sum",
    )(hbm_only(keep), recv)


def project_kernel(parts_ref, p_ref, out_ref):
    tiles = []
    for member in range(3):
        both = jnp.dot(
            parts_ref[member],
            p_ref[:, pl.ds(member * 256, 256)],
            preferred_element_type=jnp.float32,
        )
        turned = both.T
        for lanes in range(2):
            tiles.append(turned[:, lanes * 128 : (lanes + 1) * 128].reshape(32, 8, 128))
    upper = lax.broadcasted_iota(jnp.int32, (32, 8, 128), 1) < 4
    for half in range(2):
        one, two, shared = tiles[3 * half : 3 * half + 3]
        for side, whole in enumerate((one, two)):
            part = shared if side == 0 else pltpu.roll(shared, 4, 1)
            piece = jnp.concatenate([whole, jnp.where(upper, part, 0.0)], axis=1)
            out_ref[:, 2 * half + side] = piece.astype(jnp.bfloat16)


def project(parts, factors):
    return pl.pallas_call(
        project_kernel,
        out_shape=jax.ShapeDtypeStruct((32, 4, 16, 128), jnp.bfloat16),
        in_specs=[vmem(), vmem()],
        out_specs=vmem(),
        compiler_params=pltpu.CompilerParams(vmem_limit_bytes=12 * MIB),
        name="project",
    )(parts, factors)


def reduce_kernel(pieces_ref, out_ref):
    own = jnp.sum(pieces_ref[...].astype(jnp.float32), axis=0)
    total = jnp.sum(own * own)
    high = total.astype(jnp.bfloat16).astype(jnp.float32)
    row = lax.broadcasted_iota(jnp.int32, own.shape, 1)
    lane = lax.broadcasted_iota(jnp.int32, own.shape, 2)
    tail = jnp.where(row == 12, high, total - high)
    value = jnp.where(row < 12, own, jnp.where((lane == 0) & (row < 14), tail, 0.0))
    out_ref[...] = jnp.broadcast_to(value.astype(jnp.bfloat16)[None], out_ref.shape)


def reduce_pieces(pieces):
    return pl.pallas_call(
        reduce_kernel,
        out_shape=jax.ShapeDtypeStruct((32, 4, 16, 128), jnp.bfloat16),
        in_specs=[vmem()],
        out_specs=vmem(),
        compiler_params=pltpu.CompilerParams(vmem_limit_bytes=8 * MIB),
        name="reduce_pieces",
    )(pieces)


def direction_of(proj, m_one, m_two, inverse):
    normed = proj * inverse
    first = beta_one * m_one + (1 - beta_one) * normed
    second = beta_two * m_two + (1 - beta_two) * normed * normed
    return first, second, (first * lax.rsqrt(second)).astype(jnp.bfloat16)


def offsets(core):
    return (0, 3 - 2 * core, 1 + 2 * core, 2)


def finish_kernel(*refs):
    place_ref, pieces_ref = refs[:2]
    p_refs = refs[2:4]
    wm_refs = (refs[4:8], refs[8:12])
    p_own_refs = refs[12:15]
    m_refs = refs[15:18]
    step_refs = refs[18:21]
    copy_refs = refs[21:24]
    new_m_refs = refs[24:27]
    proj_ref, dir_ref, p_buf, wm_buf, p_own_buf, m_buf, turn_buf = refs[27:34]
    out_bufs = refs[34:37]
    p_sem, wm_sem, small_sem, out_sem = refs[37:]
    z, y, core = place_ref[0], place_ref[1], place_ref[2]
    slots = (core, 1 - core)
    mine = (z * 4 + y) * 2 + core
    levels = [[lax.rem(z + d, 4) for d in offsets(slot)] for slot in slots]
    columns = [[lax.rem(y + d, 4) for d in offsets(slot)] for slot in slots]

    wm_copies = []
    p_copies = []
    for array in range(4):
        for side in range(2):
            copy = pltpu.make_async_copy(
                wm_refs[side][array],
                wm_buf.at[side, pl.ds(4 * array, 4)],
                wm_sem.at[array * 2 + side],
            )
            copy.start()
            wm_copies.append(copy)
    small = []
    for member in range(3):
        for refs_of, buf, sem in ((m_refs, m_buf, member), (p_own_refs, p_own_buf, 3 + member)):
            copy = pltpu.make_async_copy(refs_of[member], buf.at[member], small_sem.at[sem])
            copy.start()
            small.append(copy)
    for array in range(4):
        for side in range(2):
            for index in range(4):
                spot = array * 4 + index
                place = levels[side][array] * 4 + columns[side][index]
                copy = pltpu.make_async_copy(
                    p_refs[side].at[place], p_buf.at[side, spot], p_sem.at[side * 16 + spot]
                )
                copy.start()
                p_copies.append(copy)

    squares = jnp.zeros((8, 128), jnp.float32)
    upper = lax.broadcasted_iota(jnp.int32, (32, 8, 128), 1) < 4
    for half in range(2):
        one = pieces_ref[:, 2 * half].astype(jnp.float32)
        two = pieces_ref[:, 2 * half + 1].astype(jnp.float32)
        tails = jnp.where(upper, 0.0, one[:, 8:] + two[:, 8:])
        squares = squares + jnp.sum(tails, axis=0)
        shared = jnp.where(upper, one[:, 8:], pltpu.roll(two[:, 8:], 4, 1))
        for tile, value in enumerate((one[:, :8], two[:, :8], shared)):
            proj_ref[:, :, pl.ds((3 * half + tile) * 128, 128)] = value
    total = jnp.sum(squares)
    inverse = lax.rsqrt(jnp.full((8, 768), total / 786432 + 1e-06))

    for array in range(4):
        for side in range(2):
            wm_copies[array * 2 + side].wait()
            for index in range(4):
                spot = array * 4 + index
                row = (levels[side][array] * 4 + columns[side][index]) * 2 + slots[side]
                dir_ref[row] = direction_of(
                    proj_ref[row],
                    wm_buf[side, spot, 64:72].astype(jnp.float32),
                    wm_buf[side, spot, 72:80].astype(jnp.float32),
                    inverse,
                )[2].astype(jnp.float32)

    directions = []
    for member in range(3):
        cols = pl.ds(member * 256, 256)
        directions.append(dir_ref[:, :, cols].reshape(256, 256).astype(jnp.bfloat16))
    outs = []
    for array in range(4):
        for side in range(2):
            for copy in p_copies[(array * 2 + side) * 4 :][:4]:
                copy.wait()
            spots = pl.ds(array * 4, 4)
            for member in range(3):
                cols = pl.ds(member * 256, 256)
                step = jnp.dot(
                    p_buf[side, spots, :, cols].reshape(256, 256),
                    directions[member],
                    preferred_element_type=jnp.float32,
                ).reshape(4, 64, 256)
                weight = wm_buf[side, spots, :64, cols].astype(jnp.float32)
                fresh = (weight - learn_rate * step).astype(jnp.bfloat16)
                target = out_bufs[member] if member < 2 else turn_buf
                for index in range(4):
                    place = levels[side][array] * 4 + columns[side][index]
                    target[place, slots[side]] = fresh[index]
                if member < 2:
                    part = pl.ds(levels[side][array] * 4, 4)
                    copy = pltpu.make_async_copy(
                        out_bufs[member].at[part, slots[side]],
                        copy_refs[member].at[part, slots[side]],
                        out_sem.at[(array * 2 + side) * 2 + member],
                    )
                    copy.start()
                    outs.append(copy)
        if array == 1:
            continue
        for done in (1, 2) if array == 2 else (array,):
            level = levels[0][done]
            for index in range(4):
                place = level * 4 + index
                lanes = pl.ds(pl.multiple_of(place * 128, 128), 128)
                out_bufs[2][:, lanes] = turn_buf[place].reshape(128, 256).T
            part = pl.ds(pl.multiple_of(level * 512, 512), 512)
            copy = pltpu.make_async_copy(
                out_bufs[2].at[:, part], copy_refs[2].at[:, part], out_sem.at[16 + done]
            )
            copy.start()
            outs.append(copy)

    for copy in small:
        copy.wait()
    for member in range(3):
        cols = pl.ds(member * 256, 256)
        first, second, _ = direction_of(
            proj_ref[mine, :, cols], m_buf[member, 0], m_buf[member, 1], inverse[:, :256]
        )
        new_m_refs[member][0] = first
        new_m_refs[member][1] = second
        step_refs[member][...] = jnp.dot(
            p_own_buf[member], directions[member], preferred_element_type=jnp.float32
        )
    for copy in outs:
        copy.wait()


def finish(place, pieces, p_a, p_b, wm_a, wm_b, p_own, moments):
    rows = pltpu.HBM((16, 2, 64, 256), jnp.bfloat16)
    turned = pltpu.HBM((256, 2048), jnp.bfloat16)
    step = jax.ShapeDtypeStruct((64, 256), jnp.float32)
    moment = jax.ShapeDtypeStruct((2, 8, 256), jnp.float32)
    fetched = [hbm_only(a) for a in (p_a, p_b, *wm_a, *wm_b, *p_own, *moments)]
    return pl.pallas_call(
        finish_kernel,
        out_shape=(step,) * 3 + (rows, rows, turned) + (moment,) * 3,
        in_specs=[smem(), vmem()] + [in_hbm()] * len(fetched),
        out_specs=(vmem(),) * 3 + (in_hbm(),) * 3 + (vmem(),) * 3,
        scratch_shapes=[
            pltpu.VMEM((32, 8, 768), jnp.float32),
            pltpu.VMEM((32, 8, 768), jnp.float32),
            pltpu.VMEM((2, 16, 64, 768), jnp.bfloat16),
            pltpu.VMEM((2, 16, 80, 768), jnp.bfloat16),
            pltpu.VMEM((3, 64, 256), jnp.bfloat16),
            pltpu.VMEM((3, 2, 8, 256), jnp.float32),
            pltpu.VMEM((16, 2, 64, 256), jnp.bfloat16),
            pltpu.VMEM((16, 2, 64, 256), jnp.bfloat16),
            pltpu.VMEM((16, 2, 64, 256), jnp.bfloat16),
            pltpu.VMEM((256, 2048), jnp.bfloat16),
            pltpu.SemaphoreType.DMA((32,)),
            pltpu.SemaphoreType.DMA((8,)),
            pltpu.SemaphoreType.DMA((6,)),
            pltpu.SemaphoreType.DMA((20,)),
        ],
        compiler_params=pltpu.CompilerParams(vmem_limit_bytes=32 * MIB),
        name="finish",
    )(place, pieces, *fetched)


def body(
    x_saved,
    h_saved,
    key_cot,
    value_cot,
    out_cot,
    w_key,
    w_value,
    w_out,
    p_key,
    p_value,
    p_out,
    m_key,
    m_value,
    m_out,
):
    place = jnp.stack([lax.axis_index(a) for a in FS]).astype(jnp.int32)
    core = place[2:]
    p_all = spread(p_key, p_value, p_out)
    p_a = lax.all_to_all(p_all, FAR, 0, 0, tiled=True)

    keep, send = grad_halves(core, key_cot, value_cot, h_saved, x_saved, out_cot)
    recv = swap(send)

    w_own = jnp.concatenate([w_key, w_value, w_out.T], axis=1)
    m_own = jnp.concatenate([m_key, m_value, m_out], axis=2).reshape(16, 768)
    wm_own = jnp.concatenate([w_own, m_own], axis=0).astype(jnp.bfloat16)
    wm_y = [wm_own] + [mirrored(wm_own, "fs_1", by) for by in (1, -1, 2)]
    wm_y = jnp.stack(wm_y)

    parts = pair_sum(keep, recv)
    partial = project(parts, p_a.reshape(1024, 768))
    pieces = lax.all_to_all(
        partial.reshape(128, 16, 128), (*FS, "tp"), 0, 0, tiled=True
    )
    wm_near = mirrored(wm_y, "fs_0", 1)
    wm_next = mirrored(wm_y, "fs_0", -1)
    p_b = swap(p_a)

    packed = reduce_pieces(pieces.reshape(32, 4, 16, 128))
    whole = lax.all_to_all(packed.reshape(128, 16, 128), (*FS, "tp"), 0, 0, tiled=True)
    wm_far = mirrored(wm_near, "fs_0", 1)
    wm_a = (wm_y, wm_near, wm_next, wm_far)
    wm_b = tuple(swap(a) for a in wm_a)
    outs = finish(
        place,
        whole.reshape(32, 4, 16, 128),
        p_a,
        p_b,
        wm_a,
        wm_b,
        (p_key, p_value, p_out),
        (m_key, m_value, m_out),
    )
    return (
        outs[0],
        outs[1],
        outs[2].T,
        outs[3].reshape(2048, 256),
        outs[4].reshape(2048, 256),
        *outs[5:],
    )


def solution(mesh):
    split = Mesh(mesh.devices.reshape(4, 4, 2, mesh.shape["tp"]), ("fs_0", "fs_1", "fs_2", "tp"))
    in_specs = (
        P(FS, None),
        P(FS, "tp"),
        P(FS, "tp"),
        P(FS, "tp"),
        P(FS, None),
        P(FS, "tp"),
        P(FS, "tp"),
        P("tp", FS),
        P(FS, None),
        P(FS, None),
        P(FS, None),
        P(None, FS, "tp"),
        P(None, FS, "tp"),
        P(None, FS, "tp"),
    )
    out_specs = (
        P(FS, "tp"),
        P(FS, "tp"),
        P("tp", FS),
        P(None, "tp"),
        P(None, "tp"),
        P("tp", None),
        P(None, FS, "tp"),
        P(None, FS, "tp"),
        P(None, FS, "tp"),
    )
    return jax.shard_map(
        body, mesh=split, in_specs=in_specs, out_specs=out_specs, check_vma=False
    )
```

```python
import jax
import jax.numpy as jnp
from jax import lax
from jax.experimental import pallas as pl
from jax.experimental.pallas import tpu as pltpu
from jax.sharding import Mesh
from jax.sharding import PartitionSpec as P

FS = ("fs_0", "fs_1", "fs_2")
FAR = ("fs_0", "fs_1")
CORE = "fs_2"
MIB = 1024 * 1024

beta_one = 0.9
beta_two = 0.9
learn_rate = 0.01


def vmem():
    return pl.BlockSpec(memory_space=pltpu.VMEM)


def smem():
    return pl.BlockSpec(memory_space=pltpu.SMEM)


def shift(value, axis, by):
    size = lax.axis_size(axis)
    return lax.ppermute(value, axis, [(i, (i + by) % size) for i in range(size)])


def crossed(value, stage, by):
    pairs = []
    for z in range(4):
        for y in range(4):
            for core in range(2):
                if stage == core:
                    target = (z, (y + by) % 4)
                else:
                    target = ((z + by) % 4, y)
                pairs.append(((z * 4 + y) * 2 + core, (target[0] * 4 + target[1]) * 2 + core))
    return lax.ppermute(value, FS, pairs)


def swap(value):
    return shift(value, CORE, 1)


def spread_kernel(a_ref, b_ref, c_ref, out_ref):
    for copy in range(16):
        for member, ref in enumerate((a_ref, b_ref, c_ref)):
            out_ref[copy, :, pl.ds(member * 256, 256)] = ref[...]


def spread(a, b, c):
    return pl.pallas_call(
        spread_kernel,
        out_shape=jax.ShapeDtypeStruct((16, 64, 768), jnp.bfloat16),
        in_specs=[vmem()] * 3,
        out_specs=vmem(),
        name="spread",
    )(a, b, c)


def split_lanes(grad, first, keep_ref, send_ref, rows, start):
    for pair in range(grad.shape[1] // 256):
        left = grad[:, pair * 256 : pair * 256 + 128]
        right = grad[:, pair * 256 + 128 : pair * 256 + 256]
        low_half = lax.broadcasted_iota(jnp.int32, left.shape, 1) < 64
        turned = pltpu.roll(jnp.where(low_half, right, left), 64, 1)
        zero = jnp.where(low_half, left, turned)
        one = jnp.where(low_half, turned, right)
        columns = pl.ds(start + pair * 128, 128)
        keep_ref[rows, columns] = jnp.where(first, zero, one).astype(jnp.bfloat16)
        send_ref[rows, columns] = jnp.where(first, one, zero).astype(jnp.bfloat16)


TILE = 1024
TILES = 2048 // TILE


def grad_kernel(
    core_ref,
    k_ref,
    v_ref,
    h_ref,
    x_ref,
    o_ref,
    keep_ref,
    send_ref,
    narrow_ref,
    wide_ref,
    keep_buf,
    send_buf,
    narrow_sem,
    wide_sem,
    out_sem,
):
    narrow = [
        pltpu.make_async_copy(ref, narrow_ref.at[n], narrow_sem.at[n])
        for n, ref in enumerate((k_ref, v_ref, h_ref))
    ]
    wide = [
        pltpu.make_async_copy(
            ref.at[:, pl.ds(tile * TILE, TILE)],
            wide_ref.at[group, :, pl.ds(tile * TILE, TILE)],
            wide_sem.at[group * TILES + tile],
        )
        for group, ref in enumerate((x_ref, o_ref))
        for tile in range(TILES)
    ]
    narrow[0].start()
    wide[0].start()
    narrow[1].start()
    for copy in wide[1:TILES]:
        copy.start()
    narrow[2].start()
    for copy in wide[TILES:]:
        copy.start()
    first = core_ref[0] == 0
    outs = []
    for group, members in enumerate(((0, 1), (2,))):
        for tile in range(TILES):
            for member in members:
                if tile == 0:
                    narrow[member].wait()
                if member == members[0]:
                    wide[group * TILES + tile].wait()
                rows = pl.ds(member * 256, 256)
                grad = lax.dot_general(
                    narrow_ref[member],
                    wide_ref[group, :, pl.ds(tile * TILE, TILE)],
                    (((0,), (0,)), ((), ())),
                    preferred_element_type=jnp.float32,
                )
                split_lanes(grad, first, keep_buf, send_buf, rows, tile * TILE // 2)
                if tile < TILES - 1:
                    continue
                for side, (buf, ref) in enumerate(((keep_buf, keep_ref), (send_buf, send_ref))):
                    copy = pltpu.make_async_copy(
                        buf.at[rows, :], ref.at[rows, :], out_sem.at[member * 2 + side]
                    )
                    copy.start()
                    outs.append(copy)
    for copy in outs:
        copy.wait()


def hbm_only(value):
    return pltpu.with_memory_space_constraint(value, pltpu.HBM)


def in_hbm():
    return pl.BlockSpec(memory_space=pltpu.HBM)


def grad_halves(core, key_cot, value_cot, h_saved, x_saved, out_cot):
    return pl.pallas_call(
        grad_kernel,
        out_shape=(
            pltpu.HBM((768, 1024), jnp.bfloat16),
            pltpu.HBM((768, 1024), jnp.bfloat16),
        ),
        in_specs=[smem()] + [in_hbm()] * 5,
        out_specs=(in_hbm(), in_hbm()),
        scratch_shapes=[
            pltpu.VMEM((3, 2048, 256), jnp.bfloat16),
            pltpu.VMEM((2, 2048, 2048), jnp.bfloat16),
            pltpu.VMEM((768, 1024), jnp.bfloat16),
            pltpu.VMEM((768, 1024), jnp.bfloat16),
            pltpu.SemaphoreType.DMA((3,)),
            pltpu.SemaphoreType.DMA((2 * TILES,)),
            pltpu.SemaphoreType.DMA((6,)),
        ],
        compiler_params=pltpu.CompilerParams(vmem_limit_bytes=48 * MIB),
        name="grads",
    )(core, *[hbm_only(a) for a in (key_cot, value_cot, h_saved, x_saved, out_cot)])


def pair_kernel(keep_ref, recv_ref, parts_ref, keep_buf, sem):
    copies = []
    for member in range(3):
        rows = pl.ds(member * 256, 256)
        copies.append(
            pltpu.make_async_copy(keep_ref.at[rows, :], keep_buf.at[rows, :], sem.at[member])
        )
        copies[member].start()
    for member in range(3):
        rows = pl.ds(member * 256, 256)
        copies[member].wait()
        grad = keep_buf[rows, :].astype(jnp.float32) + recv_ref[rows, :].astype(jnp.float32)
        parts_ref[member] = grad.astype(jnp.bfloat16)


def pair_sum(keep, recv):
    return pl.pallas_call(
        pair_kernel,
        out_shape=jax.ShapeDtypeStruct((3, 256, 1024), jnp.bfloat16),
        in_specs=[in_hbm(), vmem()],
        out_specs=vmem(),
        scratch_shapes=[
            pltpu.VMEM((768, 1024), jnp.bfloat16),
            pltpu.SemaphoreType.DMA((3,)),
        ],
        compiler_params=pltpu.CompilerParams(vmem_limit_bytes=12 * MIB),
        name="pair_sum",
    )(hbm_only(keep), recv)


def project_kernel(core_ref, parts_ref, p_ref, mine_ref, other_ref, other_buf, sem):
    first = core_ref[0] == 0
    tiles = []
    upper = lax.broadcasted_iota(jnp.int32, (16, 2, 8, 128), 2) < 4
    copies = []
    for member in range(3):
        both = jnp.dot(
            parts_ref[member],
            p_ref[:, pl.ds(member * 256, 256)],
            preferred_element_type=jnp.float32,
        )
        turned = both.T
        for lanes in range(2):
            tiles.append(turned[:, lanes * 128 : (lanes + 1) * 128].reshape(16, 2, 8, 128))
        if member == 0:
            continue
        half = member - 1
        one, two, shared = tiles[3 * half : 3 * half + 3]
        for side, whole in enumerate((one, two)):
            part = shared if side == 0 else pltpu.roll(shared, 4, 2)
            piece = jnp.concatenate([whole, jnp.where(upper, part, 0.0)], axis=2)
            mine_ref[:, 2 * half + side] = jnp.where(first, piece[:, 0], piece[:, 1])
            other_buf[half, :, side] = jnp.where(first, piece[:, 1], piece[:, 0]).astype(
                jnp.bfloat16
            )
        copy = pltpu.make_async_copy(
            other_buf.at[half], other_ref.at[:, pl.ds(2 * half, 2)], sem.at[half]
        )
        copy.start()
        copies.append(copy)
    for copy in copies:
        copy.wait()


def project(core, parts, factors):
    return pl.pallas_call(
        project_kernel,
        out_shape=(
            jax.ShapeDtypeStruct((16, 4, 16, 128), jnp.float32),
            pltpu.HBM((16, 4, 16, 128), jnp.bfloat16),
        ),
        in_specs=[smem(), vmem(), vmem()],
        out_specs=(vmem(), in_hbm()),
        scratch_shapes=[
            pltpu.VMEM((2, 16, 2, 16, 128), jnp.bfloat16),
            pltpu.SemaphoreType.DMA((2,)),
        ],
        compiler_params=pltpu.CompilerParams(vmem_limit_bytes=12 * MIB),
        name="project",
    )(core, parts, factors)


def reduce_kernel(pieces_ref, out_ref):
    own = jnp.sum(pieces_ref[...].astype(jnp.float32), axis=0)
    total = jnp.sum(own * own)
    high = total.astype(jnp.bfloat16).astype(jnp.float32)
    row = lax.broadcasted_iota(jnp.int32, own.shape, 1)
    lane = lax.broadcasted_iota(jnp.int32, own.shape, 2)
    tail = jnp.where(row == 12, high, total - high)
    value = jnp.where(row < 12, own, jnp.where((lane == 0) & (row < 14), tail, 0.0))
    out_ref[...] = jnp.broadcast_to(value.astype(jnp.bfloat16)[None], out_ref.shape)


def reduce_pieces(pieces):
    return pl.pallas_call(
        reduce_kernel,
        out_shape=jax.ShapeDtypeStruct((16, 4, 16, 128), jnp.bfloat16),
        in_specs=[vmem()],
        out_specs=vmem(),
        compiler_params=pltpu.CompilerParams(vmem_limit_bytes=8 * MIB),
        name="reduce_pieces",
    )(pieces)


def direction_of(proj, m_one, m_two, inverse):
    normed = proj * inverse
    first = beta_one * m_one + (1 - beta_one) * normed
    second = beta_two * m_two + (1 - beta_two) * normed * normed
    return first, second, (first * lax.rsqrt(second)).astype(jnp.bfloat16)


ORDER = (0, 3, 1, 2)


def finish_kernel(*refs):
    place_ref, *piece_refs = refs[:3]
    refs = refs[1:]
    p_refs = refs[2:4]
    wm_refs = (refs[4:9], refs[9:14])
    p_own_refs = refs[14:17]
    m_refs = refs[17:20]
    step_refs = refs[20:23]
    copy_refs = refs[23:26]
    new_m_refs = refs[26:29]
    proj_ref, dir_ref, p_buf, wm_buf, p_own_buf, m_buf, turn_buf = refs[29:36]
    out_bufs = refs[36:39]
    whole_ref, moment_buf, step_buf, level_ref = refs[39:43]
    p_sem, wm_sem, small_sem, out_sem = refs[43:]
    z, y, core = place_ref[0], place_ref[1], place_ref[2]
    slots = (core, 1 - core)
    mine = (z * 4 + y) * 2 + core
    levels = [lax.rem(z + d, 4) for d in ORDER]
    columns = [lax.rem(y + d, 4) for d in ORDER]

    for index in range(4):
        level_ref[index] = levels[index]

    def wm_copy(side, array, turned):
        parts = pl.ds(0, 4) if array < 3 else pl.ds(0, 2) if array == 3 else pl.ds(2, 2)
        lead = min(array, 3)
        buf = wm_buf.at[side, parts, lead] if turned else wm_buf.at[side, lead, parts]
        return pltpu.make_async_copy(wm_refs[side][array], buf, wm_sem.at[side * 5 + array])

    for turned in (False, True):

        @pl.when((core == 1) == turned)
        def _():
            for array in range(5):
                wm_copy(0, array, turned).start()
                wm_copy(1, array, not turned).start()

    small = []
    for member in range(3):
        for refs_of, buf, sem in ((m_refs, m_buf, member), (p_own_refs, p_own_buf, 3 + member)):
            copy = pltpu.make_async_copy(refs_of[member], buf.at[member], small_sem.at[sem])
            copy.start()
            small.append(copy)
    p_copy = pltpu.make_async_copy(p_refs[1], p_buf, p_sem.at[0])
    p_copy.start()

    squares = jnp.zeros((8, 128), jnp.float32)
    upper = lax.broadcasted_iota(jnp.int32, (16, 8, 128), 1) < 4
    for half in range(2):
        for slot, pieces_ref in zip(slots, piece_refs):
            one = pieces_ref[:, 2 * half].astype(jnp.float32)
            two = pieces_ref[:, 2 * half + 1].astype(jnp.float32)
            tails = jnp.where(upper, 0.0, one[:, 8:] + two[:, 8:])
            squares = squares + jnp.sum(tails, axis=0)
            shared = jnp.where(upper, one[:, 8:], pltpu.roll(two[:, 8:], 4, 1))
            for tile, value in enumerate((one[:, :8], two[:, :8], shared)):
                lanes = pl.ds((3 * half + tile) * 128, 128)
                for index in range(16):
                    proj_ref[index * 2 + slot, :, lanes] = value[index]
    total = jnp.sum(squares)
    inverse = lax.rsqrt(jnp.full((8, 768), total / 786432 + 1e-06))

    for array in range(5):
        for side in range(2):
            wm_copy(side, array, False).wait()

    @pl.loop(0, 4)
    def _(turn):
        for side in range(2):
            for index in range(4):
                row = (level_ref[turn] * 4 + columns[index]) * 2 + slots[side]
                dir_ref[row] = direction_of(
                    proj_ref[row],
                    wm_buf[side, turn, index, 64:72].astype(jnp.float32),
                    wm_buf[side, turn, index, 72:80].astype(jnp.float32),
                    inverse,
                )[2].astype(jnp.float32)

    for member in range(3):
        cols = pl.ds(member * 256, 256)
        whole_ref[member] = dir_ref[:, :, cols].reshape(256, 256).astype(jnp.bfloat16)
    for copy in small:
        copy.wait()
    small_outs = []
    for member in range(3):
        cols = pl.ds(member * 256, 256)
        first, second, _ = direction_of(
            proj_ref[mine, :, cols], m_buf[member, 0], m_buf[member, 1], inverse[:, :256]
        )
        moment_buf[member, 0] = first
        moment_buf[member, 1] = second
        step_buf[member] = jnp.dot(
            p_own_buf[member], whole_ref[member], preferred_element_type=jnp.float32
        )
        for index, (buf, target) in enumerate(
            ((moment_buf, new_m_refs[member]), (step_buf, step_refs[member]))
        ):
            copy = pltpu.make_async_copy(
                buf.at[member], target, small_sem.at[6 + member * 2 + index]
            )
            copy.start()
            small_outs.append(copy)
    p_copy.wait()

    def out_copy(turn, level, member):
        if member < 2:
            part = pl.ds(level * 4, 4)
            source, target = out_bufs[member].at[part], copy_refs[member].at[part]
        else:
            part = pl.ds(pl.multiple_of(level * 512, 512), 512)
            source, target = out_bufs[2].at[:, part], copy_refs[2].at[:, part]
        return pltpu.make_async_copy(source, target, out_sem.at[turn * 3 + member])

    @pl.loop(0, 4)
    def _(turn):
        level = level_ref[turn]
        places = [level * 4 + column for column in columns]
        for member in range(3):
            cols = pl.ds(member * 256, 256)
            for side, p_ref in enumerate((p_refs[0], p_buf)):
                factor = jnp.concatenate([p_ref[place, :, cols] for place in places], axis=0)
                step = jnp.dot(
                    factor, whole_ref[member], preferred_element_type=jnp.float32
                ).reshape(4, 64, 256)
                weight = wm_buf[side, turn, :, :64, cols].astype(jnp.float32)
                fresh = (weight - learn_rate * step).astype(jnp.bfloat16)
                target = out_bufs[member] if member < 2 else turn_buf
                for index, place in enumerate(places):
                    target[place, slots[side]] = fresh[index]
            if member == 2:
                for index in range(4):
                    place = level * 4 + index
                    lanes = pl.ds(pl.multiple_of(place * 128, 128), 128)
                    out_bufs[2][:, lanes] = turn_buf[place].reshape(128, 256).T
            out_copy(turn, level, member).start()

    for copy in small_outs:
        copy.wait()
    for turn in range(4):
        for member in range(3):
            out_copy(turn, level_ref[turn], member).wait()


def finish(place, pieces, others, p_a, p_b, wm_a, wm_b, p_own, moments):
    rows = pltpu.HBM((16, 2, 64, 256), jnp.bfloat16)
    turned = pltpu.HBM((256, 2048), jnp.bfloat16)
    step = pltpu.HBM((64, 256), jnp.float32)
    moment = pltpu.HBM((2, 8, 256), jnp.float32)
    fetched = [hbm_only(a) for a in (p_b, *wm_a, *wm_b, *p_own, *moments)]
    return pl.pallas_call(
        finish_kernel,
        out_shape=(step,) * 3 + (rows, rows, turned) + (moment,) * 3,
        in_specs=[smem(), vmem(), vmem(), vmem()] + [in_hbm()] * len(fetched),
        out_specs=(in_hbm(),) * 9,
        scratch_shapes=[
            pltpu.VMEM((32, 8, 768), jnp.float32),
            pltpu.VMEM((32, 8, 768), jnp.float32),
            pltpu.VMEM((16, 64, 768), jnp.bfloat16),
            pltpu.VMEM((2, 4, 4, 80, 768), jnp.bfloat16),
            pltpu.VMEM((3, 64, 256), jnp.bfloat16),
            pltpu.VMEM((3, 2, 8, 256), jnp.float32),
            pltpu.VMEM((16, 2, 64, 256), jnp.bfloat16),
            pltpu.VMEM((16, 2, 64, 256), jnp.bfloat16),
            pltpu.VMEM((16, 2, 64, 256), jnp.bfloat16),
            pltpu.VMEM((256, 2048), jnp.bfloat16),
            pltpu.VMEM((3, 256, 256), jnp.bfloat16),
            pltpu.VMEM((3, 2, 8, 256), jnp.float32),
            pltpu.VMEM((3, 64, 256), jnp.float32),
            pltpu.SMEM((4,), jnp.int32),
            pltpu.SemaphoreType.DMA((1,)),
            pltpu.SemaphoreType.DMA((10,)),
            pltpu.SemaphoreType.DMA((12,)),
            pltpu.SemaphoreType.DMA((12,)),
        ],
        compiler_params=pltpu.CompilerParams(vmem_limit_bytes=32 * MIB),
        name="finish",
    )(place, pieces, others, p_a, *fetched)


def body(
    x_saved,
    h_saved,
    key_cot,
    value_cot,
    out_cot,
    w_key,
    w_value,
    w_out,
    p_key,
    p_value,
    p_out,
    m_key,
    m_value,
    m_out,
):
    place = jnp.stack([lax.axis_index(a) for a in FS]).astype(jnp.int32)
    core = place[2:]
    p_all = spread(p_key, p_value, p_out)
    p_a = lax.all_to_all(p_all, FAR, 0, 0, tiled=True)

    keep, send = grad_halves(core, key_cot, value_cot, h_saved, x_saved, out_cot)
    recv = swap(send)

    w_own = jnp.concatenate([w_key, w_value, w_out.T], axis=1)
    m_own = jnp.concatenate([m_key, m_value, m_out], axis=2).reshape(16, 768)
    wm_own = jnp.concatenate([w_own, m_own], axis=0).astype(jnp.bfloat16)
    line = [wm_own] + [crossed(wm_own, 0, by) for by in (1, -1, 2)]
    line = jnp.stack(line)

    parts = pair_sum(keep, recv)
    mine, other = project(core, parts, p_a.reshape(1024, 768))
    partial = (mine + swap(other).astype(jnp.float32)).astype(jnp.bfloat16)
    pieces = lax.all_to_all(
        partial.reshape(64, 16, 128), (*FAR, "tp"), 0, 0, tiled=True
    )
    near = crossed(line, 1, 1)
    after = crossed(line, 1, -1)
    p_b = swap(p_a)

    packed = reduce_pieces(pieces.reshape(16, 4, 16, 128))
    whole = lax.all_to_all(packed.reshape(64, 16, 128), (*FAR, "tp"), 0, 0, tiled=True)
    whole = whole.reshape(16, 4, 16, 128)
    others = swap(whole)
    far_one = crossed(near[:2], 1, 1)
    far_two = crossed(after[2:], 1, -1)
    wm_a = (line, near, after, far_one, far_two)
    wm_b = [swap(a) for a in wm_a[:3]]
    wm_b += [swap(a) for a in wm_a[3:]]
    outs = finish(
        place,
        whole,
        others,
        p_a,
        p_b,
        wm_a,
        wm_b,
        (p_key, p_value, p_out),
        (m_key, m_value, m_out),
    )
    return (
        outs[0],
        outs[1],
        outs[2].T,
        outs[3].reshape(2048, 256),
        outs[4].reshape(2048, 256),
        *outs[5:],
    )


def solution(mesh):
    split = Mesh(mesh.devices.reshape(4, 4, 2, mesh.shape["tp"]), ("fs_0", "fs_1", "fs_2", "tp"))
    in_specs = (
        P(FS, None),
        P(FS, "tp"),
        P(FS, "tp"),
        P(FS, "tp"),
        P(FS, None),
        P(FS, "tp"),
        P(FS, "tp"),
        P("tp", FS),
        P(FS, None),
        P(FS, None),
        P(FS, None),
        P(None, FS, "tp"),
        P(None, FS, "tp"),
        P(None, FS, "tp"),
    )
    out_specs = (
        P(FS, "tp"),
        P(FS, "tp"),
        P("tp", FS),
        P(None, "tp"),
        P(None, "tp"),
        P("tp", None),
        P(None, FS, "tp"),
        P(None, FS, "tp"),
        P(None, FS, "tp"),
    )
    return jax.shard_map(body, mesh=split, in_specs=in_specs, out_specs=out_specs, check_vma=False)
```

```python
import jax
import jax.numpy as jnp
from jax import lax
from jax.experimental import pallas as pl
from jax.experimental.pallas import tpu as pltpu
from jax.sharding import Mesh
from jax.sharding import PartitionSpec as P

FS = ("fs_0", "fs_1", "fs_2")
FAR = ("fs_0", "fs_1")
CORE = "fs_2"
MIB = 1024 * 1024

beta_one = 0.9
beta_two = 0.9
learn_rate = 0.01


def vmem():
    return pl.BlockSpec(memory_space=pltpu.VMEM)


def smem():
    return pl.BlockSpec(memory_space=pltpu.SMEM)


def shift(value, axis, by):
    size = lax.axis_size(axis)
    return lax.ppermute(value, axis, [(i, (i + by) % size) for i in range(size)])


def crossed(value, stage, by):
    pairs = []
    for z in range(4):
        for y in range(4):
            for core in range(2):
                if stage == core:
                    target = (z, (y + by) % 4)
                else:
                    target = ((z + by) % 4, y)
                pairs.append(((z * 4 + y) * 2 + core, (target[0] * 4 + target[1]) * 2 + core))
    return lax.ppermute(value, FS, pairs)


def swap(value):
    return shift(value, CORE, 1)


def spread_kernel(a_ref, b_ref, c_ref, out_ref):
    for copy in range(16):
        for member, ref in enumerate((a_ref, b_ref, c_ref)):
            out_ref[copy, :, pl.ds(member * 256, 256)] = ref[...]


def spread(a, b, c):
    return pl.pallas_call(
        spread_kernel,
        out_shape=jax.ShapeDtypeStruct((16, 64, 768), jnp.bfloat16),
        in_specs=[vmem()] * 3,
        out_specs=vmem(),
        name="spread",
    )(a, b, c)


def split_lanes(grad, first, keep_ref, send_ref, rows, start):
    for pair in range(grad.shape[1] // 256):
        left = grad[:, pair * 256 : pair * 256 + 128]
        right = grad[:, pair * 256 + 128 : pair * 256 + 256]
        low_half = lax.broadcasted_iota(jnp.int32, left.shape, 1) < 64
        turned = pltpu.roll(jnp.where(low_half, right, left), 64, 1)
        zero = jnp.where(low_half, left, turned)
        one = jnp.where(low_half, turned, right)
        columns = pl.ds(start + pair * 128, 128)
        keep_ref[rows, columns] = jnp.where(first, zero, one).astype(jnp.bfloat16)
        send_ref[rows, columns] = jnp.where(first, one, zero).astype(jnp.bfloat16)


TILE = 1024
TILES = 2048 // TILE


def grad_kernel(
    core_ref,
    k_ref,
    v_ref,
    h_ref,
    x_ref,
    o_ref,
    keep_ref,
    send_ref,
    narrow_ref,
    wide_ref,
    keep_buf,
    send_buf,
    narrow_sem,
    wide_sem,
    out_sem,
):
    narrow = [
        pltpu.make_async_copy(ref, narrow_ref.at[n], narrow_sem.at[n])
        for n, ref in enumerate((k_ref, v_ref, h_ref))
    ]
    wide = [
        pltpu.make_async_copy(
            ref.at[:, pl.ds(tile * TILE, TILE)],
            wide_ref.at[group, :, pl.ds(tile * TILE, TILE)],
            wide_sem.at[group * TILES + tile],
        )
        for group, ref in enumerate((x_ref, o_ref))
        for tile in range(TILES)
    ]
    narrow[0].start()
    wide[0].start()
    narrow[1].start()
    for copy in wide[1:TILES]:
        copy.start()
    narrow[2].start()
    for copy in wide[TILES:]:
        copy.start()
    first = core_ref[0] == 0
    outs = []
    for group, members in enumerate(((0, 1), (2,))):
        for tile in range(TILES):
            for member in members:
                if tile == 0:
                    narrow[member].wait()
                if member == members[0]:
                    wide[group * TILES + tile].wait()
                rows = pl.ds(member * 256, 256)
                grad = lax.dot_general(
                    narrow_ref[member],
                    wide_ref[group, :, pl.ds(tile * TILE, TILE)],
                    (((0,), (0,)), ((), ())),
                    preferred_element_type=jnp.float32,
                )
                split_lanes(grad, first, keep_buf, send_buf, rows, tile * TILE // 2)
                if tile < TILES - 1:
                    continue
                for side, (buf, ref) in enumerate(((keep_buf, keep_ref), (send_buf, send_ref))):
                    copy = pltpu.make_async_copy(
                        buf.at[rows, :], ref.at[rows, :], out_sem.at[member * 2 + side]
                    )
                    copy.start()
                    outs.append(copy)
    for copy in outs:
        copy.wait()


def hbm_only(value):
    return pltpu.with_memory_space_constraint(value, pltpu.HBM)


def in_hbm():
    return pl.BlockSpec(memory_space=pltpu.HBM)


def grad_halves(core, key_cot, value_cot, h_saved, x_saved, out_cot):
    return pl.pallas_call(
        grad_kernel,
        out_shape=(
            pltpu.HBM((768, 1024), jnp.bfloat16),
            pltpu.HBM((768, 1024), jnp.bfloat16),
        ),
        in_specs=[smem()] + [in_hbm()] * 5,
        out_specs=(in_hbm(), in_hbm()),
        scratch_shapes=[
            pltpu.VMEM((3, 2048, 256), jnp.bfloat16),
            pltpu.VMEM((2, 2048, 2048), jnp.bfloat16),
            pltpu.VMEM((768, 1024), jnp.bfloat16),
            pltpu.VMEM((768, 1024), jnp.bfloat16),
            pltpu.SemaphoreType.DMA((3,)),
            pltpu.SemaphoreType.DMA((2 * TILES,)),
            pltpu.SemaphoreType.DMA((6,)),
        ],
        compiler_params=pltpu.CompilerParams(vmem_limit_bytes=48 * MIB),
        name="grads",
    )(core, *[hbm_only(a) for a in (key_cot, value_cot, h_saved, x_saved, out_cot)])


def pair_kernel(keep_ref, recv_ref, parts_ref, keep_buf, sem):
    copies = []
    for member in range(3):
        rows = pl.ds(member * 256, 256)
        copies.append(
            pltpu.make_async_copy(keep_ref.at[rows, :], keep_buf.at[rows, :], sem.at[member])
        )
        copies[member].start()
    for member in range(3):
        rows = pl.ds(member * 256, 256)
        copies[member].wait()
        grad = keep_buf[rows, :].astype(jnp.float32) + recv_ref[rows, :].astype(jnp.float32)
        parts_ref[member] = grad.astype(jnp.bfloat16)


def pair_sum(keep, recv):
    return pl.pallas_call(
        pair_kernel,
        out_shape=jax.ShapeDtypeStruct((3, 256, 1024), jnp.bfloat16),
        in_specs=[in_hbm(), vmem()],
        out_specs=vmem(),
        scratch_shapes=[
            pltpu.VMEM((768, 1024), jnp.bfloat16),
            pltpu.SemaphoreType.DMA((3,)),
        ],
        compiler_params=pltpu.CompilerParams(vmem_limit_bytes=12 * MIB),
        name="pair_sum",
    )(hbm_only(keep), recv)


def project_kernel(core_ref, parts_ref, p_ref, mine_ref, other_ref, other_buf, sem):
    first = core_ref[0] == 0
    tiles = []
    upper = lax.broadcasted_iota(jnp.int32, (16, 2, 8, 128), 2) < 4
    copies = []
    for member in range(3):
        both = jnp.dot(
            parts_ref[member],
            p_ref[:, pl.ds(member * 256, 256)],
            preferred_element_type=jnp.float32,
        )
        turned = both.T
        for lanes in range(2):
            tiles.append(turned[:, lanes * 128 : (lanes + 1) * 128].reshape(16, 2, 8, 128))
        if member == 0:
            continue
        half = member - 1
        one, two, shared = tiles[3 * half : 3 * half + 3]
        for side, whole in enumerate((one, two)):
            part = shared if side == 0 else pltpu.roll(shared, 4, 2)
            piece = jnp.concatenate([whole, jnp.where(upper, part, 0.0)], axis=2)
            mine_ref[:, 2 * half + side] = jnp.where(first, piece[:, 0], piece[:, 1])
            other_buf[half, :, side] = jnp.where(first, piece[:, 1], piece[:, 0]).astype(
                jnp.bfloat16
            )
        copy = pltpu.make_async_copy(
            other_buf.at[half], other_ref.at[:, pl.ds(2 * half, 2)], sem.at[half]
        )
        copy.start()
        copies.append(copy)
    for copy in copies:
        copy.wait()


def project(core, parts, factors):
    return pl.pallas_call(
        project_kernel,
        out_shape=(
            jax.ShapeDtypeStruct((16, 4, 16, 128), jnp.float32),
            pltpu.HBM((16, 4, 16, 128), jnp.bfloat16),
        ),
        in_specs=[smem(), vmem(), vmem()],
        out_specs=(vmem(), in_hbm()),
        scratch_shapes=[
            pltpu.VMEM((2, 16, 2, 16, 128), jnp.bfloat16),
            pltpu.SemaphoreType.DMA((2,)),
        ],
        compiler_params=pltpu.CompilerParams(vmem_limit_bytes=12 * MIB),
        name="project",
    )(core, parts, factors)


def reduce_kernel(pieces_ref, out_ref):
    own = jnp.sum(pieces_ref[...].astype(jnp.float32), axis=0)
    total = jnp.sum(own * own)
    high = total.astype(jnp.bfloat16).astype(jnp.float32)
    row = lax.broadcasted_iota(jnp.int32, own.shape, 1)
    lane = lax.broadcasted_iota(jnp.int32, own.shape, 2)
    tail = jnp.where(row == 12, high, total - high)
    value = jnp.where(row < 12, own, jnp.where((lane == 0) & (row < 14), tail, 0.0))
    out_ref[...] = jnp.broadcast_to(value.astype(jnp.bfloat16)[None], out_ref.shape)


def reduce_pieces(pieces):
    return pl.pallas_call(
        reduce_kernel,
        out_shape=jax.ShapeDtypeStruct((16, 4, 16, 128), jnp.bfloat16),
        in_specs=[vmem()],
        out_specs=vmem(),
        compiler_params=pltpu.CompilerParams(vmem_limit_bytes=8 * MIB),
        name="reduce_pieces",
    )(pieces)


def line_kernel(own_ref, below_ref, above_ref, across_ref, one_ref, two_ref):
    one_ref[0] = own_ref[...]
    one_ref[1] = below_ref[...]
    two_ref[0] = above_ref[...]
    two_ref[1] = across_ref[...]


def join_line(*blocks):
    half = jax.ShapeDtypeStruct((2, 80, 768), jnp.bfloat16)
    return pl.pallas_call(
        line_kernel,
        out_shape=(half, half),
        in_specs=[vmem()] * 4,
        out_specs=(vmem(),) * 2,
        compiler_params=pltpu.CompilerParams(vmem_limit_bytes=8 * MIB),
        name="join_line",
    )(*blocks)


def direction_of(proj, m_one, m_two, inverse):
    normed = proj * inverse
    first = beta_one * m_one + (1 - beta_one) * normed
    second = beta_two * m_two + (1 - beta_two) * normed * normed
    return first, second, (first * lax.rsqrt(second)).astype(jnp.bfloat16)


ORDER = (0, 3, 1, 2)


def finish_kernel(*refs):
    place_ref, *piece_refs = refs[:3]
    refs = refs[1:]
    p_refs = refs[2:4]
    wm_refs = (refs[4:12], refs[12:20])
    p_own_refs = refs[20:23]
    m_refs = refs[23:26]
    step_refs = refs[26:29]
    copy_refs = refs[29:32]
    new_m_refs = refs[32:35]
    proj_ref, dir_ref, p_buf, wm_buf, p_own_buf, m_buf, turn_buf = refs[35:42]
    out_bufs = refs[42:45]
    whole_ref, moment_buf, step_buf, level_ref = refs[45:49]
    p_sem, wm_sem, small_sem, out_sem = refs[49:]
    z, y, core = place_ref[0], place_ref[1], place_ref[2]
    slots = (core, 1 - core)
    mine = (z * 4 + y) * 2 + core
    levels = [lax.rem(z + d, 4) for d in ORDER]
    columns = [lax.rem(y + d, 4) for d in ORDER]

    for index in range(4):
        level_ref[index] = levels[index]

    def wm_copy(side, array, turned):
        parts, lead = pl.ds(array % 2 * 2, 2), array // 2
        buf = wm_buf.at[side, parts, lead] if turned else wm_buf.at[side, lead, parts]
        return pltpu.make_async_copy(wm_refs[side][array], buf, wm_sem.at[side * 8 + array])

    for turned in (False, True):

        @pl.when((core == 1) == turned)
        def _():
            for array in range(8):
                wm_copy(0, array, turned).start()
                wm_copy(1, array, not turned).start()

    small = []
    for member in range(3):
        for refs_of, buf, sem in ((m_refs, m_buf, member), (p_own_refs, p_own_buf, 3 + member)):
            copy = pltpu.make_async_copy(refs_of[member], buf.at[member], small_sem.at[sem])
            copy.start()
            small.append(copy)
    p_copy = pltpu.make_async_copy(p_refs[1], p_buf, p_sem.at[0])
    p_copy.start()

    squares = jnp.zeros((8, 128), jnp.float32)
    upper = lax.broadcasted_iota(jnp.int32, (16, 8, 128), 1) < 4
    for half in range(2):
        for slot, pieces_ref in zip(slots, piece_refs):
            one = pieces_ref[:, 2 * half].astype(jnp.float32)
            two = pieces_ref[:, 2 * half + 1].astype(jnp.float32)
            tails = jnp.where(upper, 0.0, one[:, 8:] + two[:, 8:])
            squares = squares + jnp.sum(tails, axis=0)
            shared = jnp.where(upper, one[:, 8:], pltpu.roll(two[:, 8:], 4, 1))
            for tile, value in enumerate((one[:, :8], two[:, :8], shared)):
                lanes = pl.ds((3 * half + tile) * 128, 128)
                for index in range(16):
                    proj_ref[index * 2 + slot, :, lanes] = value[index]
    total = jnp.sum(squares)
    inverse = lax.rsqrt(jnp.full((8, 768), total / 786432 + 1e-06))

    for array in range(8):
        for side in range(2):
            wm_copy(side, array, False).wait()

    @pl.loop(0, 4)
    def _(turn):
        for side in range(2):
            for index in range(4):
                row = (level_ref[turn] * 4 + columns[index]) * 2 + slots[side]
                dir_ref[row] = direction_of(
                    proj_ref[row],
                    wm_buf[side, turn, index, 64:72].astype(jnp.float32),
                    wm_buf[side, turn, index, 72:80].astype(jnp.float32),
                    inverse,
                )[2].astype(jnp.float32)

    for member in range(3):
        cols = pl.ds(member * 256, 256)
        whole_ref[member] = dir_ref[:, :, cols].reshape(256, 256).astype(jnp.bfloat16)
    for copy in small:
        copy.wait()
    small_outs = []
    for member in range(3):
        cols = pl.ds(member * 256, 256)
        first, second, _ = direction_of(
            proj_ref[mine, :, cols], m_buf[member, 0], m_buf[member, 1], inverse[:, :256]
        )
        moment_buf[member, 0] = first
        moment_buf[member, 1] = second
        step_buf[member] = jnp.dot(
            p_own_buf[member], whole_ref[member], preferred_element_type=jnp.float32
        )
        for index, (buf, target) in enumerate(
            ((moment_buf, new_m_refs[member]), (step_buf, step_refs[member]))
        ):
            copy = pltpu.make_async_copy(
                buf.at[member], target, small_sem.at[6 + member * 2 + index]
            )
            copy.start()
            small_outs.append(copy)
    p_copy.wait()

    def out_copy(turn, level, member):
        if member < 2:
            part = pl.ds(level * 4, 4)
            source, target = out_bufs[member].at[part], copy_refs[member].at[part]
        else:
            part = pl.ds(pl.multiple_of(level * 512, 512), 512)
            source, target = out_bufs[2].at[:, part], copy_refs[2].at[:, part]
        return pltpu.make_async_copy(source, target, out_sem.at[turn * 3 + member])

    @pl.loop(0, 4)
    def _(turn):
        level = level_ref[turn]
        places = [level * 4 + column for column in columns]
        for member in (2, 0, 1):
            cols = pl.ds(member * 256, 256)
            for side, p_ref in enumerate((p_refs[0], p_buf)):
                factor = jnp.concatenate([p_ref[place, :, cols] for place in places], axis=0)
                step = jnp.dot(
                    factor, whole_ref[member], preferred_element_type=jnp.float32
                ).reshape(4, 64, 256)
                weight = wm_buf[side, turn, :, :64, cols].astype(jnp.float32)
                fresh = (weight - learn_rate * step).astype(jnp.bfloat16)
                target = out_bufs[member] if member < 2 else turn_buf
                for index, place in enumerate(places):
                    target[place, slots[side]] = fresh[index]
            if member == 2:
                for index in range(4):
                    place = level * 4 + index
                    lanes = pl.ds(pl.multiple_of(place * 128, 128), 128)
                    out_bufs[2][:, lanes] = turn_buf[place].reshape(128, 256).T
            out_copy(turn, level, member).start()

    for copy in small_outs:
        copy.wait()
    for turn in range(4):
        for member in range(3):
            out_copy(turn, level_ref[turn], member).wait()


def finish(place, pieces, others, p_a, p_b, wm_a, wm_b, p_own, moments):
    rows = pltpu.HBM((16, 2, 64, 256), jnp.bfloat16)
    turned = pltpu.HBM((256, 2048), jnp.bfloat16)
    step = pltpu.HBM((64, 256), jnp.float32)
    moment = pltpu.HBM((2, 8, 256), jnp.float32)
    fetched = [hbm_only(a) for a in (p_b, *wm_a, *wm_b, *p_own, *moments)]
    return pl.pallas_call(
        finish_kernel,
        out_shape=(step,) * 3 + (rows, rows, turned) + (moment,) * 3,
        in_specs=[smem(), vmem(), vmem(), vmem()] + [in_hbm()] * len(fetched),
        out_specs=(in_hbm(),) * 9,
        scratch_shapes=[
            pltpu.VMEM((32, 8, 768), jnp.float32),
            pltpu.VMEM((32, 8, 768), jnp.float32),
            pltpu.VMEM((16, 64, 768), jnp.bfloat16),
            pltpu.VMEM((2, 4, 4, 80, 768), jnp.bfloat16),
            pltpu.VMEM((3, 64, 256), jnp.bfloat16),
            pltpu.VMEM((3, 2, 8, 256), jnp.float32),
            pltpu.VMEM((16, 2, 64, 256), jnp.bfloat16),
            pltpu.VMEM((16, 2, 64, 256), jnp.bfloat16),
            pltpu.VMEM((16, 2, 64, 256), jnp.bfloat16),
            pltpu.VMEM((256, 2048), jnp.bfloat16),
            pltpu.VMEM((3, 256, 256), jnp.bfloat16),
            pltpu.VMEM((3, 2, 8, 256), jnp.float32),
            pltpu.VMEM((3, 64, 256), jnp.float32),
            pltpu.SMEM((4,), jnp.int32),
            pltpu.SemaphoreType.DMA((1,)),
            pltpu.SemaphoreType.DMA((16,)),
            pltpu.SemaphoreType.DMA((12,)),
            pltpu.SemaphoreType.DMA((12,)),
        ],
        compiler_params=pltpu.CompilerParams(vmem_limit_bytes=32 * MIB),
        name="finish",
    )(place, pieces, others, p_a, *fetched)


def body(
    x_saved,
    h_saved,
    key_cot,
    value_cot,
    out_cot,
    w_key,
    w_value,
    w_out,
    p_key,
    p_value,
    p_out,
    m_key,
    m_value,
    m_out,
):
    place = jnp.stack([lax.axis_index(a) for a in FS]).astype(jnp.int32)
    core = place[2:]
    p_all = spread(p_key, p_value, p_out)
    p_a = lax.all_to_all(p_all, FAR, 0, 0, tiled=True)

    keep, send = grad_halves(core, key_cot, value_cot, h_saved, x_saved, out_cot)
    recv = swap(send)

    w_own = jnp.concatenate([w_key, w_value, w_out.T], axis=1)
    m_own = jnp.concatenate([m_key, m_value, m_out], axis=2).reshape(16, 768)
    wm_own = jnp.concatenate([w_own, m_own], axis=0).astype(jnp.bfloat16)
    below = crossed(wm_own, 0, 1)
    above = crossed(wm_own, 0, -1)
    across = crossed(wm_own, 0, 2)
    line_one, line_two = join_line(wm_own, below, above, across)

    parts = pair_sum(keep, recv)
    mine, other = project(core, parts, p_a.reshape(1024, 768))
    partial = (mine + swap(other).astype(jnp.float32)).astype(jnp.bfloat16)
    pieces = lax.all_to_all(
        partial.reshape(64, 16, 128), (*FAR, "tp"), 0, 0, tiled=True
    )
    near_one = crossed(line_one, 1, 1)
    after_two = crossed(line_two, 1, -1)
    near_two = crossed(line_two, 1, 1)
    after_one = crossed(line_one, 1, -1)
    p_b = swap(p_a)

    packed = reduce_pieces(pieces.reshape(16, 4, 16, 128))
    whole = lax.all_to_all(packed.reshape(64, 16, 128), (*FAR, "tp"), 0, 0, tiled=True)
    whole = whole.reshape(16, 4, 16, 128)
    others = swap(whole)
    far_one = crossed(near_one, 1, 1)
    far_two = crossed(after_two, 1, -1)
    wm_a = (line_one, line_two, near_one, near_two, after_one, after_two, far_one, far_two)
    wm_b = [swap(a) for a in wm_a[:6]]
    wm_b += [swap(a) for a in wm_a[6:]]
    outs = finish(
        place,
        whole,
        others,
        p_a,
        p_b,
        wm_a,
        wm_b,
        (p_key, p_value, p_out),
        (m_key, m_value, m_out),
    )
    return (
        outs[0],
        outs[1],
        outs[2].T,
        outs[3].reshape(2048, 256),
        outs[4].reshape(2048, 256),
        *outs[5:],
    )


def solution(mesh):
    split = Mesh(mesh.devices.reshape(4, 4, 2, mesh.shape["tp"]), ("fs_0", "fs_1", "fs_2", "tp"))
    in_specs = (
        P(FS, None),
        P(FS, "tp"),
        P(FS, "tp"),
        P(FS, "tp"),
        P(FS, None),
        P(FS, "tp"),
        P(FS, "tp"),
        P("tp", FS),
        P(FS, None),
        P(FS, None),
        P(FS, None),
        P(None, FS, "tp"),
        P(None, FS, "tp"),
        P(None, FS, "tp"),
    )
    out_specs = (
        P(FS, "tp"),
        P(FS, "tp"),
        P("tp", FS),
        P(None, "tp"),
        P(None, "tp"),
        P("tp", None),
        P(None, FS, "tp"),
        P(None, FS, "tp"),
        P(None, FS, "tp"),
    )
    return jax.shard_map(body, mesh=split, in_specs=in_specs, out_specs=out_specs, check_vma=False)
```
